32 devices in a mesh: ep: 8 (over z, x), tp: 4 (over y, core).
Axes of the slice: x: 2, y: 2, z: 4, core: 2. Of those that a mesh axis runs over, the one named last changes fastest.
Arguments:
- stream: bfloat16 [128, 4096], P(None, 'ep'), may hold values from -6.5 to 6.5
- norm_gain: float32 [4096], P('ep'), may hold values from 0.1 to 1.9
- w_query: bfloat16 [4096, 2048], P('ep', 'tp'), may hold values from -0.09375 to 0.09375
- w_key: bfloat16 [4096, 1024], P('ep', 'tp'), may hold values from -0.09375 to 0.09375
- w_value: bfloat16 [4096, 1024], P('ep', 'tp'), may hold values from -0.09375 to 0.09375
- break_offset: float32 [16], P('tp'), may hold values from -10 to -2
- cache_keys: bfloat16 [128, 1024, 8, 128], P('ep', None, 'tp'), may hold values from -6 to 6
- cache_values: bfloat16 [128, 1024, 8, 128], P('ep', None, 'tp'), may hold values from -6 to 6
- lengths: int32 [128], P('ep'), may hold values from 128 to 1024
- w_output: bfloat16 [2048, 4096], P('tp', 'ep'), may hold values from -0.125 to 0.125
- head_gain: float32 [2048], P('tp'), may hold values from 0.1 to 1.9
- ffn_gain: float32 [4096], P('ep'), may hold values from 0.1 to 1.9
- route_experts: int32 [128, 2], replicated, may hold values from 0 to 7, all different within a row; in each aligned block of 128 rows (0 to 127, 128 to 255, ...) at most 64 rows name the same one
- route_weights: float32 [128, 2], replicated, may hold values from 0.1 to 1
- expert_gate: bfloat16 [8, 4096, 1024], P('ep', None, 'tp'), may hold values from -0.09375 to 0.09375
- expert_up: bfloat16 [8, 4096, 1024], P('ep', None, 'tp'), may hold values from -0.09375 to 0.09375
- expert_down: bfloat16 [8, 1024, 4096], P('ep', 'tp'), may hold values from -0.1875 to 0.1875
- dense_gate: bfloat16 [4096, 4096], P('ep', 'tp'), may hold values from -0.09375 to 0.09375
- dense_up: bfloat16 [4096, 4096], P('ep', 'tp'), may hold values from -0.09375 to 0.09375
- dense_down: bfloat16 [4096, 4096], P('tp', 'ep'), may hold values from -0.09375 to 0.09375
- mix_gain: float32 [4096], P('ep'), may hold values from 0.1 to 1.9
Outputs:
- mixed_out: bfloat16 [128, 4096], P(None, 'ep')
- key_rows: bfloat16 [128, 1024], P('ep', 'tp')
- value_rows: bfloat16 [128, 1024], P('ep', 'tp')
The draws below stay inside these ranges and needn't reach their ends.
Inputs may be any that keep to these rules, and one draw needn't show every extreme that they name: `route_experts`: in the whole batch no expert is named by more than 64 pairs, a bound that some block reaches; the 2 experts of a token differ.
All inputs are finite; a program needn't handle non-finite values.
Results may differ from the reference program's by a relative error of at most 0.025.
Values may be sent and summed in bfloat16 or wider, within the bound.
A program may use at most 64 MiB of HBM per device.

```python
import math
import jax
import jax.numpy as jnp
import numpy as np
from jax import lax

D = 4096
HEADS = 16
KVH = 8
HD = 128
FF = 1024
FD = 4096
TOP_K = 2
LEN = 1024
SEQS = 128
EXPERTS = 8
CAP = 64
N_TP = 4


def draw_stream(key, part):
    columns = jnp.arange(D, dtype=jnp.float32) / D
    col_scale = 0.6 * jnp.power(3.0, columns)[None, :]
    base_draw = jnp.clip(jax.random.normal(key, (SEQS, D), jnp.float32), -3.3, 3.3)
    values = base_draw * col_scale
    return values.astype(jnp.bfloat16)


def draw_break_offset(key, part):
    centre = -jnp.log(jnp.float32(LEN))
    spread = jax.random.uniform(jax.random.fold_in(key, 7), (HEADS,), jnp.float32, -1.2, 0.8)
    return (centre + spread).astype(jnp.float32)


def plant(drawn, key, low, high):
    dims = drawn.shape
    place = [jax.random.randint(jax.random.fold_in(key, axis), (), 0, dims[axis]) for axis in range(len(dims))]
    drawn = drawn.at[tuple(place)].set(low)
    longest = dims.index(max(dims))
    place[longest] = (place[longest] + 1) % dims[longest]
    return drawn.at[tuple(place)].set(high)


def levels(rng, shape, split, smallest, top_value):
    def one(dim, blocks):
        steps = jax.random.uniform(jax.random.fold_in(jax.random.fold_in(rng, 6), dim), (blocks,), jnp.float32, smallest / len(split), top_value / len(split))
        return jnp.repeat(jnp.exp(steps), shape[dim] // blocks).reshape((-1,) + (1,) * (len(shape) - dim - 1))

    loudness = one(*split[0])
    for cut in split[1:]:
        loudness = loudness * one(*cut)
    return loudness


def assign_block(rng, own, number, rows, count, top, bound, lean):
    sequence = jax.random.permutation(rng, count)
    crowded, ordinary = portions_of(count, rows * top, bound, lean, True), portions_of(count, rows * top, bound, lean, False)
    places = jnp.arange(count)

    def named(tallies, offset_by):
        used = int((tallies > 0).sum())
        fixed = max(1, used // 4)
        moved = fixed + (places - fixed + offset_by * (used - fixed)) % max(1, count - fixed)
        return jnp.zeros((count,), jnp.int32).at[sequence[jnp.where(places < fixed, places, moved)]].set(jnp.asarray(tallies, jnp.int32))

    tallies = jnp.where(number % 4 == 0, named(crowded, number // 4), named(ordinary, number - number // 4 - 1))
    mixed = jax.random.permutation(jax.random.fold_in(own, 3), count)
    donor, sink = mixed[0:count // 2 * 2:2], mixed[1:count // 2 * 2:2]
    margin = jnp.minimum(tallies[donor] - 1, bound - tallies[sink]) // 2
    margin = jnp.where((donor == sequence[0]) | (sink == sequence[0]) | (tallies[sink] == 0), 0, jnp.maximum(margin, 0))
    moved = jax.random.randint(jax.random.fold_in(own, 4), (count // 2,), 0, 1 << 20) % (margin + 1)
    tallies = tallies.at[donor].add(-moved).at[sink].add(moved)
    members = jnp.searchsorted(jnp.cumsum(tallies), jnp.arange(rows * top), side="right").astype(jnp.int32)
    listing = members.reshape(top, rows).T
    listing = listing[jax.random.permutation(jax.random.fold_in(own, 1), rows)]
    offset_by = jax.random.randint(jax.random.fold_in(own, 2), (rows, 1), 0, top)
    return jnp.take_along_axis(listing, (jnp.arange(top)[None, :] + offset_by) % top, axis=1)


def portions_of(count, total, most, lean, full):
    portions = [(1 << 20) // math.isqrt(rank ** lean) + 1 for rank in range(1, count + 1)]
    largest = most if full else min(most, max(-(-total // count), total * portions[0] // sum(portions)))
    least = 1 if total - largest >= count - 1 else 0
    given, rest = [largest] + [least] * (count - 1), total - largest - least * (count - 1)
    while rest > 0:
        movable = [i for i in range(1, count) if given[i] < largest] or [i for i in range(1, count) if given[i] < most]
        pool, budget = sum([portions[i] for i in movable]), rest
        for i in movable:
            addition = min(most - given[i], max(1, budget * portions[i] // pool), rest)
            given[i] = given[i] + addition
            rest = rest - addition
    return np.array(given)


def normal_values(stream_key, extent, deviation, limit, pieces=(), kind=jnp.bfloat16):
    array = jax.random.normal(stream_key, extent, jnp.float32) * deviation
    if len(pieces) > 0:
        array = levels(stream_key, extent, pieces, -0.22, 0.18) * array
    return jnp.clip(array, min=-limit, max=limit).astype(kind)


def setup_inputs(seed: int = 0) -> dict:
    arg_keys = jax.random.split(jax.random.key(seed), 22)
    stream = draw_stream(jax.random.fold_in(arg_keys[21], 71), 0)
    norm_gain = jnp.clip(1.0 + 0.18 * jax.random.normal(arg_keys[1], (D,), jnp.float32), 0.1, 1.9)
    w_query = normal_values(arg_keys[2], (D, HEADS * HD), D ** -0.5, 0.09375, ((0, 8), (1, 4)))
    w_key = normal_values(arg_keys[3], (D, KVH * HD), D ** -0.5, 0.09375, ((0, 8), (1, 4)))
    w_value = normal_values(arg_keys[4], (D, KVH * HD), D ** -0.5, 0.09375, ((0, 8), (1, 4)))
    break_offset = draw_break_offset(jax.random.fold_in(arg_keys[21], 71), 0)
    cache_keys = normal_values(arg_keys[6], (SEQS, LEN, KVH, HD), 1.0, 6.0, ((0, 8), (2, 4)))
    cache_values = normal_values(arg_keys[7], (SEQS, LEN, KVH, HD), 1.0, 6.0, ((0, 8), (2, 4)))
    lengths = plant(jax.random.randint(arg_keys[8], (SEQS,), LEN // 8, LEN + 1), jax.random.fold_in(arg_keys[8], 1), LEN // 8, LEN).astype(jnp.int32)
    w_output = normal_values(arg_keys[9], (HEADS * HD, D), (HEADS * HD) ** -0.5, 0.125, ((0, 4), (1, 8)))
    head_gain = jnp.clip(1.0 + 0.18 * jax.random.normal(arg_keys[10], (HEADS * HD,), jnp.float32), 0.1, 1.9)
    ffn_gain = jnp.clip(1.0 + 0.18 * jax.random.normal(arg_keys[11], (D,), jnp.float32), 0.1, 1.9)
    route_experts_keys = jax.random.split(jax.random.fold_in(arg_keys[12], 1), SEQS // SEQS)
    route_experts_turns = jax.random.permutation(jax.random.fold_in(arg_keys[12], 3), SEQS // SEQS)
    route_experts = jax.vmap(lambda own, number: assign_block(jax.random.fold_in(arg_keys[12], 2), own, number, SEQS, EXPERTS, TOP_K, CAP, 2))(route_experts_keys, route_experts_turns).reshape((SEQS, TOP_K))
    route_weights = jnp.clip(jax.random.uniform(arg_keys[13], (SEQS, TOP_K), jnp.float32, 0.1, 1.0), 0.1, 1.0)
    expert_gate = normal_values(arg_keys[14], (EXPERTS, D, FF), D ** -0.5, 0.09375, ((0, 8), (2, 4)))
    expert_up = normal_values(arg_keys[15], (EXPERTS, D, FF), D ** -0.5, 0.09375, ((0, 8), (2, 4)))
    expert_down = normal_values(arg_keys[16], (EXPERTS, FF, D), FF ** -0.5, 0.1875, ((0, 8), (1, 4)))
    dense_gate = normal_values(arg_keys[17], (D, FD), D ** -0.5, 0.09375, ((0, 8), (1, 4)))
    dense_up = normal_values(arg_keys[18], (D, FD), D ** -0.5, 0.09375, ((0, 8), (1, 4)))
    dense_down = normal_values(arg_keys[19], (FD, D), FD ** -0.5, 0.09375, ((0, 4), (1, 8)))
    mix_gain = jnp.clip(1.0 + 0.18 * jax.random.normal(arg_keys[20], (D,), jnp.float32), 0.1, 1.9)
    return {"stream": stream, "norm_gain": norm_gain, "w_query": w_query, "w_key": w_key, "w_value": w_value, "break_offset": break_offset, "cache_keys": cache_keys, "cache_values": cache_values, "lengths": lengths, "w_output": w_output, "head_gain": head_gain, "ffn_gain": ffn_gain, "route_experts": route_experts, "route_weights": route_weights, "expert_gate": expert_gate, "expert_up": expert_up, "expert_down": expert_down, "dense_gate": dense_gate, "dense_up": dense_up, "dense_down": dense_down, "mix_gain": mix_gain}


EPSILON = 1e-06

def rms_rows(values, gain_vec):
    return values * lax.rsqrt(lax.optimization_barrier(jnp.mean(values * values, axis=1, keepdims=True)) + EPSILON) * gain_vec[None, :]

def narrow_sum(left_side, right_side):
    per_group = right_side.shape[0] // N_TP
    summed = jnp.zeros((left_side.shape[0], right_side.shape[1]), jnp.float32)
    for group_index in range(N_TP):
        partial_value = jnp.dot(left_side[:, group_index * per_group:(group_index + 1) * per_group], right_side[group_index * per_group:(group_index + 1) * per_group], preferred_element_type=jnp.float32)
        rounded = lax.optimization_barrier(partial_value.astype(jnp.bfloat16))
        summed = summed + rounded.astype(jnp.float32)
    return summed.astype(jnp.bfloat16)

def slot_table(route_experts, experts, capacity):
    chosen = route_experts.reshape(-1)
    onehot = (chosen[:, None] == jnp.arange(experts, dtype=jnp.int32)[None, :]).astype(jnp.int32)
    earlier = jnp.cumsum(onehot, axis=0) - onehot
    rank_in = lax.optimization_barrier(jnp.sum(earlier * onehot, axis=1)).astype(jnp.int32)
    slot_ids = (chosen * capacity + rank_in).astype(jnp.int32)
    owners = jnp.arange(chosen.shape[0], dtype=jnp.int32) // route_experts.shape[1]
    filled = jnp.full((experts * capacity,), route_experts.shape[0], jnp.int32).at[slot_ids].set(owners)
    return (slot_ids, filled)

def reference(stream, norm_gain, w_query, w_key, w_value, break_offset, cache_keys, cache_values, lengths, w_output, head_gain, ffn_gain, route_experts, route_weights, expert_gate, expert_up, expert_down, dense_gate, dense_up, dense_down, mix_gain):
    streamf = stream.astype(jnp.float32)
    normed = rms_rows(streamf, norm_gain).astype(jnp.bfloat16)
    queries = jnp.dot(normed, w_query, preferred_element_type=jnp.float32).astype(jnp.bfloat16)
    key_rows = jnp.dot(normed, w_key, preferred_element_type=jnp.float32).astype(jnp.bfloat16)
    value_rows = jnp.dot(normed, w_value, preferred_element_type=jnp.float32).astype(jnp.bfloat16)
    seq_total = stream.shape[0]
    heads = break_offset.shape[0]
    kv_heads = cache_keys.shape[2]
    head_dim = cache_keys.shape[3]
    group_size = heads // kv_heads
    offsets = break_offset.reshape(kv_heads, group_size)[:, :, None]
    gains = head_gain.reshape(kv_heads, group_size, head_dim)

    def attend(inputs):
        query_one, keys_one, values_one, length_one = inputs
        scores = jnp.einsum('kgd,lkd->kgl', query_one.astype(jnp.float32), keys_one.astype(jnp.float32))
        scores = scores * head_dim ** (-0.5) + offsets
        in_cache = (jnp.arange(keys_one.shape[0], dtype=jnp.int32) < length_one)[None, None, :]
        failed = jnp.where(in_cache, jax.nn.log_sigmoid(-scores), 0.0)
        later_sum = lax.cumsum(failed, axis=2, reverse=True) - failed
        weights = jnp.where(in_cache, jnp.exp(jax.nn.log_sigmoid(scores) + later_sum), 0.0).astype(jnp.bfloat16)
        attended = jnp.einsum('kgl,lkd->kgd', weights.astype(jnp.float32), values_one.astype(jnp.float32))
        normalized = attended * lax.rsqrt(lax.optimization_barrier(jnp.mean(attended * attended, axis=2, keepdims=True)) + EPSILON) * gains
        return normalized.astype(jnp.bfloat16).reshape(heads * head_dim)
    head_out = lax.map(attend, (queries.reshape(seq_total, kv_heads, group_size, head_dim), cache_keys, cache_values, lengths))
    attn_out = narrow_sum(head_out, w_output)
    residual = streamf + attn_out.astype(jnp.float32)
    normed_ffn = rms_rows(residual, ffn_gain).astype(jnp.bfloat16)
    gate_part = jnp.dot(normed_ffn, dense_gate, preferred_element_type=jnp.float32)
    up_part = jnp.dot(normed_ffn, dense_up, preferred_element_type=jnp.float32)
    dense_hidden = (jax.nn.silu(gate_part) * up_part).astype(jnp.bfloat16)
    dense_out = narrow_sum(dense_hidden, dense_down)
    experts = expert_gate.shape[0]
    slot_ids, filled = slot_table(route_experts, experts, CAP)
    padded = jnp.concatenate([normed_ffn, jnp.zeros((1, normed_ffn.shape[1]), jnp.bfloat16)], axis=0)
    expert_in = padded[filled].reshape(experts, CAP, normed_ffn.shape[1])

    def expert_one(inputs):
        rows_in, gate_one, up_one, down_one = inputs
        gate_val = jnp.dot(rows_in, gate_one, preferred_element_type=jnp.float32)
        up_val = jnp.dot(rows_in, up_one, preferred_element_type=jnp.float32)
        expert_hidden = (jax.nn.silu(gate_val) * up_val).astype(jnp.bfloat16)
        return narrow_sum(expert_hidden, down_one)
    expert_out = lax.map(expert_one, (expert_in, expert_gate, expert_up, expert_down))
    picked = expert_out.reshape(experts * CAP, -1)[slot_ids].reshape(seq_total, route_experts.shape[1], -1)
    shares = route_weights / lax.optimization_barrier(jnp.sum(route_weights, axis=1, keepdims=True))
    moe_out = lax.optimization_barrier(jnp.sum(picked.astype(jnp.float32) * shares[:, :, None], axis=1))
    mixed_out = (residual + moe_out + mix_gain[None, :] * dense_out.astype(jnp.float32)).astype(jnp.bfloat16)
    return (mixed_out, key_rows, value_rows)
```

```python
import functools

import jax
import jax.numpy as jnp
from jax import lax
from jax.experimental import pallas as pl
from jax.experimental.pallas import tpu as pltpu
from jax.sharding import PartitionSpec as P

EPSILON = 1e-06
MESH = pl.DeviceIdType.MESH
F32 = jnp.float32
BF16 = jnp.bfloat16
NT = (((1,), (1,)), ((), ()))


def row_sums(squares):
    ones = jnp.ones((8, squares.shape[1]), BF16)
    high = squares.astype(BF16)
    low = (squares - high.astype(F32)).astype(BF16)
    return lax.dot_general(ones, high, NT, preferred_element_type=F32) + lax.dot_general(
        ones, low, NT, preferred_element_type=F32
    )


def own_column(sums, first, rows):
    width = sums.shape[1]
    lane = lax.broadcasted_iota(jnp.int32, (rows, width), 1)
    row = lax.broadcasted_iota(jnp.int32, (rows, width), 0)
    return jnp.sum(jnp.where(lane == row + first, sums[0:1, :], 0.0), axis=1, keepdims=True)


def greet(axes):
    barrier = pltpu.get_barrier_semaphore()
    total = 0
    for axis, count in axes:
        me = lax.axis_index(axis)
        for k in range(1, count):
            pl.semaphore_signal(
                barrier, inc=1, device_id={axis: lax.rem(me + k, count)}, device_id_type=MESH
            )
            total += 1
    pl.semaphore_wait(barrier, total)


def send(axis, count, k, src, dst, send_sem, recv_sem):
    peer = lax.rem(lax.axis_index(axis) + k, count)
    copy = pltpu.make_async_remote_copy(
        src_ref=src,
        dst_ref=dst,
        send_sem=send_sem.at[k - 1],
        recv_sem=recv_sem.at[k - 1],
        device_id={axis: peer},
        device_id_type=MESH,
    )
    copy.start()
    return copy


def project_kernel(
    n, width, x_ref, g_ref, wq_ref, wk_ref, wv_ref, q_ref, k_ref, v_ref,
    part, sums, got, got_sums, s_send, s_recv, p_send, p_recv,
):
    me = lax.axis_index("ep")
    x = x_ref[...].astype(F32)
    xg = (x * g_ref[...]).astype(BF16)
    rows = k_ref.shape[0]
    sums[...] = row_sums(x * x)
    at = 0
    for w_ref in (wq_ref, wk_ref, wv_ref):
        cols = w_ref.shape[1]
        val = jnp.dot(xg, w_ref[...], preferred_element_type=F32).astype(BF16)
        for i in range(n):
            part[i, :, at : at + cols] = val[i * rows : (i + 1) * rows]
        at += cols
    greet((("ep", n),))
    copies = []
    for k in range(1, n):
        peer = lax.rem(me + k, n)
        copies.append(send("ep", n, k, part.at[peer], got.at[k - 1], p_send, p_recv))
        copies.append(send("ep", n, k, sums, got_sums.at[k - 1], s_send, s_recv))
    total = part[me].astype(F32)
    squares = sums[...]
    for k in range(1, n):
        copies[2 * k - 2].wait_recv()
        total = total + got[k - 1].astype(F32)
        copies[2 * k - 1].wait_recv()
        squares = squares + got_sums[k - 1]
    mean = own_column(squares, me * rows, rows) / width
    total = total * lax.rsqrt(mean + EPSILON)
    hd = q_ref.shape[2]
    q_width = wq_ref.shape[1]
    k_width = wk_ref.shape[1]
    for h in range(q_ref.shape[0]):
        q_ref[h] = total[:, h * hd : (h + 1) * hd].astype(BF16).astype(F32)
    k_ref[...] = total[:, q_width : q_width + k_width].astype(BF16)
    v_ref[...] = total[:, q_width + k_width :].astype(BF16)
    for copy in copies:
        copy.wait_send()


def attend_kernel(kv, per, len_ref, off_ref, q_ref, gain_ref, key_ref, val_ref, out_ref):
    step = pl.program_id(0)
    heads = q_ref.shape[0]
    hd = q_ref.shape[2]
    cols = key_ref.shape[1]
    group = heads // kv
    rows = per * heads
    lanes = 128
    blocks = cols // lanes
    q = jnp.concatenate(
        [q_ref[h, pl.ds(step * per + s, 1), :] for s in range(per) for h in range(heads)], axis=0
    ).astype(BF16)
    row = lax.broadcasted_iota(jnp.int32, (rows, lanes), 0)
    lane = lax.broadcasted_iota(jnp.int32, (rows, lanes), 1)
    offset = jnp.zeros((rows, lanes), F32)
    length = jnp.zeros((rows, lanes), jnp.int32)
    for s in range(per):
        length = jnp.where(row // heads == s, len_ref[step * per + s], length)
    for h in range(heads):
        offset = jnp.where(row % heads == h, off_ref[h], offset)
    mine = (row % heads) // group
    scores = jnp.zeros((rows, cols), F32)
    row_all = lax.broadcasted_iota(jnp.int32, (rows, cols), 0)
    for s in range(per):
        one = lax.dot_general(q, key_ref[s], NT, preferred_element_type=F32)
        scores = one if s == 0 else jnp.where(row_all // heads == s, one, scores)
    sigs, valids, fails = [], [], []
    for b in range(blocks):
        sc = scores[:, b * lanes : (b + 1) * lanes] * hd ** (-0.5) + offset
        col = lane + b * lanes
        valid = (col // kv < length) & (col % kv == mine)
        ls = jnp.minimum(sc, 0.0) - jnp.log(1.0 + jnp.exp(-jnp.abs(sc)))
        sigs.append(ls)
        valids.append(valid)
        fails.append(jnp.where(valid, ls - sc, 0.0))
    failed = jnp.concatenate(fails, axis=0)
    high = failed.astype(BF16)
    low = (failed - high.astype(F32)).astype(BF16)
    r = lax.broadcasted_iota(jnp.int32, (lanes, 2 * lanes), 0)
    c = lax.broadcasted_iota(jnp.int32, (lanes, 2 * lanes), 1)
    tri = jnp.where((r > c) | (c >= lanes), 1.0, 0.0).astype(BF16)
    sums = jnp.dot(high, tri, preferred_element_type=F32) + jnp.dot(
        low, tri, preferred_element_type=F32
    )
    acc = jnp.zeros((rows, lanes), F32)
    weights = [None] * blocks
    for b in reversed(range(blocks)):
        later = sums[b * rows : (b + 1) * rows, :lanes] + acc
        acc = acc + sums[b * rows : (b + 1) * rows, lanes:]
        weights[b] = jnp.where(valids[b], jnp.exp(sigs[b] + later), 0.0)
    weights = jnp.concatenate(weights, axis=1).astype(BF16)
    row_out = lax.broadcasted_iota(jnp.int32, (rows, hd), 0)
    att = None
    for s in range(per):
        one = jnp.dot(weights, val_ref[s], preferred_element_type=F32)
        att = one if s == 0 else jnp.where(row_out // heads == s, one, att)
    gains = jnp.concatenate([gain_ref[...]] * per, axis=0)
    att = att * lax.rsqrt(jnp.mean(att * att, axis=1, keepdims=True) + EPSILON) * gains
    for s in range(per):
        for h in range(heads):
            out_ref[h, pl.ds(step * per + s, 1), :] = att[s * heads + h : s * heads + h + 1]


def rest_kernel(
    n, nt, width, cap,
    head_ref, x_ref, fg_ref, mix_ref, slot_row_ref, share_row_ref, slot_col_ref,
    wo_hbm, dg_hbm, du_hbm, dd_hbm, eg_hbm, eu_hbm, ed_hbm,
    out_ref,
    wo, dg, du, dd, eg, eu, ed, w_sem,
    heads_all, part, parts, disp, disp_in, sums, sums_in, gu, gu_in, hid_all, ret, ret_in,
    fin, fins,
    h_send, h_recv, a_send, a_recv, d_send, d_recv, s_send, s_recv, g_send, g_recv,
    i_send, i_recv, r_send, r_recv, f_send, f_recv,
):
    me = lax.axis_index("ep")
    loads = []
    for i, (src, dst) in enumerate(
        ((wo_hbm, wo), (dg_hbm, dg), (du_hbm, du), (eg_hbm.at[0], eg), (eu_hbm.at[0], eu),
         (ed_hbm.at[0], ed), (dd_hbm, dd))
    ):
        load = pltpu.make_async_copy(src, dst, w_sem.at[i])
        load.start()
        loads.append(load)
    total_rows, block = x_ref.shape
    rows = total_rows // n
    heads_all[me] = jnp.concatenate(
        [head_ref[h] for h in range(head_ref.shape[0])], axis=1
    ).astype(BF16)
    greet((("ep", n), ("tp", nt)))
    sent = []
    copies = [
        send("ep", n, k, heads_all.at[me], heads_all.at[me], h_send, h_recv) for k in range(1, n)
    ]
    sent += copies
    slot_rows = lax.broadcasted_iota(jnp.int32, (cap, total_rows), 0)
    loads[0].wait()
    for copy in copies:
        copy.wait_recv()
    all_heads = heads_all[...].reshape(total_rows, heads_all.shape[2])
    part[...] = jnp.dot(all_heads, wo[...], preferred_element_type=F32).astype(BF16)
    copies = [send("tp", nt, k, part, parts.at[k - 1], a_send, a_recv) for k in range(1, nt)]
    sent += copies
    attn = part[...].astype(F32)
    for k in range(1, nt):
        copies[k - 1].wait_recv()
        attn = attn + parts[k - 1].astype(F32)
    residual = x_ref[...].astype(F32) + attn.astype(BF16).astype(F32)
    u = (residual * fg_ref[...]).astype(BF16)
    sums[...] = row_sums(residual * residual)
    slots = [slot_row_ref[k : k + 1, :] for k in range(slot_row_ref.shape[0])]

    def picks(expert):
        place = slot_rows + expert * cap
        return [slot == place for slot in slots]

    d_copies, s_copies = [], []
    for k in range(1, n):
        peer = lax.rem(me + k, n)
        hit = functools.reduce(jnp.logical_or, picks(peer))
        disp[k] = jnp.dot(
            jnp.where(hit, 1.0, 0.0).astype(BF16), u, preferred_element_type=F32
        ).astype(BF16)
        d_copies.append(send("ep", n, k, disp.at[k], disp_in.at[k - 1], d_send, d_recv))
        s_copies.append(send("ep", n, k, sums, sums_in.at[k - 1], s_send, s_recv))
    sent += d_copies + s_copies
    mine = picks(me)
    hit = functools.reduce(jnp.logical_or, mine)
    own_in = jnp.dot(
        jnp.where(hit, 1.0, 0.0).astype(BF16), u, preferred_element_type=F32
    ).astype(BF16)
    hidden = dg.shape[1]
    loads[1].wait()
    val = jnp.dot(u, dg[...], preferred_element_type=F32).astype(BF16)
    for i in range(n):
        gu[i, :, :hidden] = val[i * rows : (i + 1) * rows]
    loads[2].wait()
    val = jnp.dot(u, du[...], preferred_element_type=F32).astype(BF16)
    for i in range(n):
        gu[i, :, hidden:] = val[i * rows : (i + 1) * rows]
    g_copies = [
        send("ep", n, k, gu.at[lax.rem(me + k, n)], gu_in.at[k - 1], g_send, g_recv)
        for k in range(1, n)
    ]
    sent += g_copies
    loads[3].wait()
    loads[4].wait()
    first = pl.ds(pl.multiple_of(me * block, block), block)
    gate = jnp.dot(own_in, eg[first, :], preferred_element_type=F32)
    up = jnp.dot(own_in, eu[first, :], preferred_element_type=F32)
    squares = sums[...]
    for k in range(1, n):
        s_copies[k - 1].wait_recv()
        squares = squares + sums_in[k - 1]
        d_copies[k - 1].wait_recv()
        owner = lax.rem(me - k + n, n)
        span = pl.ds(pl.multiple_of(owner * block, block), block)
        gate = gate + jnp.dot(disp_in[k - 1], eg[span, :], preferred_element_type=F32)
        up = up + jnp.dot(disp_in[k - 1], eu[span, :], preferred_element_type=F32)
    scale_row = lax.rsqrt(squares[0:1, :] / width + EPSILON)
    scale = jnp.sum(jnp.where(hit, scale_row, 0.0), axis=1, keepdims=True)
    share = jnp.zeros((cap, 1), F32)
    for k in range(len(mine)):
        share = share + jnp.sum(
            jnp.where(mine[k], share_row_ref[k : k + 1, :], 0.0), axis=1, keepdims=True
        )
    gate = gate * scale
    up = up * scale
    act = (gate / (1.0 + jnp.exp(-gate)) * up).astype(BF16)
    loads[5].wait()
    for i in range(n):
        ret[i] = (
            jnp.dot(act, ed[:, i * block : (i + 1) * block], preferred_element_type=F32) * share
        ).astype(BF16)
    r_copies = [
        send("ep", n, k, ret.at[lax.rem(me + k, n)], ret_in.at[k - 1], r_send, r_recv)
        for k in range(1, n)
    ]
    sent += r_copies
    gate_up = gu[me].astype(F32)
    for k in range(1, n):
        g_copies[k - 1].wait_recv()
        gate_up = gate_up + gu_in[k - 1].astype(F32)
    gate_up = gate_up * own_column(
        jnp.broadcast_to(scale_row, (8, total_rows)), me * rows, rows
    )
    dense_gate = gate_up[:, :hidden]
    hid_all[me] = (dense_gate / (1.0 + jnp.exp(-dense_gate)) * gate_up[:, hidden:]).astype(BF16)
    i_copies = [
        send("ep", n, k, hid_all.at[me], hid_all.at[me], i_send, i_recv) for k in range(1, n)
    ]
    sent += i_copies
    slot_cols = lax.broadcasted_iota(jnp.int32, (total_rows, cap), 1)
    columns = [slot_col_ref[:, k : k + 1] for k in range(slot_col_ref.shape[1])]

    def combine(expert, rows_in):
        place = slot_cols + expert * cap
        hits = functools.reduce(jnp.logical_or, [column == place for column in columns])
        return jnp.dot(
            jnp.where(hits, 1.0, 0.0).astype(BF16), rows_in, preferred_element_type=F32
        )

    moe = combine(me, ret[me])
    for k in range(1, n):
        r_copies[k - 1].wait_recv()
        moe = moe + combine(lax.rem(me - k + n, n), ret_in[k - 1])
    loads[6].wait()
    for copy in i_copies:
        copy.wait_recv()
    dense = jnp.dot(
        hid_all[...].reshape(total_rows, hidden), dd[...], preferred_element_type=F32
    )
    both = moe + mix_ref[...] * dense
    fin[...] = both.astype(BF16)
    f_copies = [send("tp", nt, k, fin, fins.at[k - 1], f_send, f_recv) for k in range(1, nt)]
    sent += f_copies
    total = residual + fin[...].astype(F32)
    for k in range(1, nt):
        f_copies[k - 1].wait_recv()
        total = total + fins[k - 1].astype(F32)
    out_ref[...] = total.astype(BF16)
    for copy in sent:
        copy.wait_send()


def per_device(
    n, nt, stream, norm_gain, w_query, w_key, w_value, break_offset, cache_keys, cache_values,
    lengths, w_output, head_gain, ffn_gain, route_experts, route_weights, expert_gate,
    expert_up, expert_down, dense_gate, dense_up, dense_down, mix_gain,
):
    total_rows, block = stream.shape
    width = block * n
    rows = lengths.shape[0]
    kv = cache_keys.shape[2]
    hd = cache_keys.shape[3]
    heads = break_offset.shape[0]
    cache_len = cache_keys.shape[1]
    top = route_experts.shape[1]
    hidden = dense_gate.shape[1]
    expert_hidden = expert_gate.shape[2]
    experts = expert_gate.shape[0] * n
    cap = 2 * rows * top // expert_gate.shape[0]
    assert experts == n
    vmem = pl.BlockSpec(memory_space=pltpu.VMEM)
    hbm = pl.BlockSpec(memory_space=pl.ANY)
    dma = pltpu.SemaphoreType.DMA
    limit = 60 * 1024 * 1024

    wide = w_query.shape[1] + w_key.shape[1] + w_value.shape[1]
    queries, key_rows, value_rows = pl.pallas_call(
        functools.partial(project_kernel, n, width),
        out_shape=(
            jax.ShapeDtypeStruct((heads, rows, hd), F32),
            jax.ShapeDtypeStruct((rows, w_key.shape[1]), BF16),
            jax.ShapeDtypeStruct((rows, w_value.shape[1]), BF16),
        ),
        in_specs=[vmem] * 5,
        out_specs=(vmem, vmem, vmem),
        scratch_shapes=[
            pltpu.VMEM((n, rows, wide), BF16),
            pltpu.VMEM((8, total_rows), F32),
            pltpu.VMEM((n - 1, rows, wide), BF16),
            pltpu.VMEM((n - 1, 8, total_rows), F32),
            dma((n - 1,)), dma((n - 1,)), dma((n - 1,)), dma((n - 1,)),
        ],
        compiler_params=pltpu.CompilerParams(collective_id=0, has_side_effects=True),
        name="project",
    )(stream, norm_gain.reshape(1, block), w_query, w_key, w_value)

    per = 2
    flat = kv * cache_len
    smem = pl.BlockSpec(memory_space=pltpu.SMEM)
    head_out = pl.pallas_call(
        functools.partial(attend_kernel, kv, per),
        grid=(rows // per,),
        out_shape=jax.ShapeDtypeStruct((heads, rows, hd), F32),
        in_specs=[
            smem,
            smem,
            pl.BlockSpec((heads, rows, hd), lambda i: (0, 0, 0)),
            pl.BlockSpec((heads, hd), lambda i: (0, 0)),
            pl.BlockSpec((per, flat, hd), lambda i: (i, 0, 0)),
            pl.BlockSpec((per, flat, hd), lambda i: (i, 0, 0)),
        ],
        out_specs=pl.BlockSpec((heads, rows, hd), lambda i: (0, 0, 0)),
        compiler_params=pltpu.CompilerParams(dimension_semantics=("arbitrary",)),
        name="attend",
    )(
        lengths,
        break_offset,
        queries,
        head_gain.reshape(heads, hd),
        cache_keys.reshape(rows, flat, hd),
        cache_values.reshape(rows, flat, hd),
    )

    chosen = route_experts.reshape(-1)
    pair = jnp.arange(chosen.shape[0], dtype=jnp.int32)
    earlier = (chosen[None, :] == chosen[:, None]) & (pair[None, :] < pair[:, None])
    slot_ids = chosen * cap + jnp.sum(earlier.astype(jnp.int32), axis=1)
    slot_ids = slot_ids.reshape(total_rows, top)
    shares = route_weights / jnp.sum(route_weights, axis=1, keepdims=True)

    dt = w_output.shape[0]
    return_shape = (n, cap, block)
    mixed_out = pl.pallas_call(
        functools.partial(rest_kernel, n, nt, width, cap),
        out_shape=jax.ShapeDtypeStruct((total_rows, block), BF16),
        in_specs=[vmem] * 7 + [hbm] * 7,
        out_specs=vmem,
        scratch_shapes=[
            pltpu.VMEM(w_output.shape, BF16),
            pltpu.VMEM(dense_gate.shape, BF16),
            pltpu.VMEM(dense_up.shape, BF16),
            pltpu.VMEM(dense_down.shape, BF16),
            pltpu.VMEM(expert_gate.shape[1:], BF16),
            pltpu.VMEM(expert_up.shape[1:], BF16),
            pltpu.VMEM(expert_down.shape[1:], BF16),
            dma((7,)),
            pltpu.VMEM((n, rows, dt), BF16),
            pltpu.VMEM((total_rows, block), BF16),
            pltpu.VMEM((nt - 1, total_rows, block), BF16),
            pltpu.VMEM(return_shape, BF16),
            pltpu.VMEM((n - 1, cap, block), BF16),
            pltpu.VMEM((8, total_rows), F32),
            pltpu.VMEM((n - 1, 8, total_rows), F32),
            pltpu.VMEM((n, rows, 2 * hidden), BF16),
            pltpu.VMEM((n - 1, rows, 2 * hidden), BF16),
            pltpu.VMEM((n, rows, hidden), BF16),
            pltpu.VMEM(return_shape, BF16),
            pltpu.VMEM((n - 1, cap, block), BF16),
            pltpu.VMEM((total_rows, block), BF16),
            pltpu.VMEM((nt - 1, total_rows, block), BF16),
            dma((n - 1,)), dma((n - 1,)), dma((nt - 1,)), dma((nt - 1,)),
            dma((n - 1,)), dma((n - 1,)), dma((n - 1,)), dma((n - 1,)),
            dma((n - 1,)), dma((n - 1,)), dma((n - 1,)), dma((n - 1,)),
            dma((n - 1,)), dma((n - 1,)), dma((nt - 1,)), dma((nt - 1,)),
        ],
        compiler_params=pltpu.CompilerParams(
            collective_id=1, has_side_effects=True, vmem_limit_bytes=limit
        ),
        name="rest",
    )(
        head_out, stream, ffn_gain.reshape(1, block), mix_gain.reshape(1, block),
        slot_ids.T, shares.T, slot_ids,
        w_output, dense_gate, dense_up, dense_down, expert_gate, expert_up, expert_down,
    )
    return (mixed_out, key_rows, value_rows)


def solution(mesh):
    in_specs = (
        P(None, "ep"),
        P("ep"),
        P("ep", "tp"),
        P("ep", "tp"),
        P("ep", "tp"),
        P("tp"),
        P("ep", None, "tp", None),
        P("ep", None, "tp", None),
        P("ep"),
        P("tp", "ep"),
        P("tp"),
        P("ep"),
        P(),
        P(),
        P("ep", None, "tp"),
        P("ep", None, "tp"),
        P("ep", "tp", None),
        P("ep", "tp"),
        P("ep", "tp"),
        P("tp", "ep"),
        P("ep"),
    )
    out_specs = (P(None, "ep"), P("ep", "tp"), P("ep", "tp"))
    body = functools.partial(per_device, mesh.shape["ep"], mesh.shape["tp"])
    return jax.shard_map(
        body, mesh=mesh, in_specs=in_specs, out_specs=out_specs, check_vma=False
    )
```

```python
import functools

import jax
import jax.numpy as jnp
from jax import lax
from jax.experimental import pallas as pl
from jax.experimental.pallas import tpu as pltpu
from jax.sharding import PartitionSpec as P

EPSILON = 1e-06
MESH = pl.DeviceIdType.MESH
F32 = jnp.float32
BF16 = jnp.bfloat16
NT = (((1,), (1,)), ((), ()))


def row_sums(squares):
    ones = jnp.ones((8, squares.shape[1]), BF16)
    high = squares.astype(BF16)
    low = (squares - high.astype(F32)).astype(BF16)
    return lax.dot_general(ones, high, NT, preferred_element_type=F32) + lax.dot_general(
        ones, low, NT, preferred_element_type=F32
    )


def own_column(sums, first, rows):
    width = sums.shape[1]
    lane = lax.broadcasted_iota(jnp.int32, (rows, width), 1)
    row = lax.broadcasted_iota(jnp.int32, (rows, width), 0)
    return jnp.sum(jnp.where(lane == row + first, sums[0:1, :], 0.0), axis=1, keepdims=True)


def greet(axes):
    barrier = pltpu.get_barrier_semaphore()
    total = 0
    for axis, count in axes:
        me = lax.axis_index(axis)
        for k in range(1, count):
            pl.semaphore_signal(
                barrier, inc=1, device_id={axis: lax.rem(me + k, count)}, device_id_type=MESH
            )
            total += 1
    pl.semaphore_wait(barrier, total)


def send(axis, count, k, src, dst, send_sem, recv_sem):
    peer = lax.rem(lax.axis_index(axis) + k, count)
    copy = pltpu.make_async_remote_copy(
        src_ref=src,
        dst_ref=dst,
        send_sem=send_sem.at[k - 1],
        recv_sem=recv_sem.at[k - 1],
        device_id={axis: peer},
        device_id_type=MESH,
    )
    copy.start()
    return copy


def send_to(peer, src, dst, sems, i):
    copy = pltpu.make_async_remote_copy(
        src_ref=src,
        dst_ref=dst,
        send_sem=sems[0].at[i],
        recv_sem=sems[1].at[i],
        device_id={"tp": peer},
        device_id_type=MESH,
    )
    copy.start()
    return copy


def tp_sum(nt, part, arrived, pair, crossed, full, sems, extra):
    me = lax.axis_index("tp")
    core = lax.rem(me, 2)
    partner = me + 1 - 2 * core
    half = pair.shape[0]
    mine = pl.ds(pl.multiple_of(core * half, half), half)
    other = pl.ds(pl.multiple_of((1 - core) * half, half), half)
    copies = [send_to(partner, part.at[other], arrived, sems, 0)]
    copies[0].wait_recv()
    pair[...] = (part[mine].astype(F32) + arrived[...].astype(F32)).astype(BF16)
    for j in range(1, nt // 2):
        copies.append(send_to(lax.rem(me + 2 * j, nt), pair, crossed.at[j - 1], sems, j))
    total = pair[...].astype(F32)
    for j in range(1, nt // 2):
        copies[j].wait_recv()
        total = total + crossed[j - 1].astype(F32)
    if extra is not None:
        total = total + extra[mine]
    full[mine] = total.astype(BF16)
    copies.append(send_to(partner, full.at[mine], full.at[mine], sems, nt // 2))
    copies[-1].wait_recv()
    for copy in copies:
        copy.wait_send()


def project_kernel(
    n, width, x_ref, g_ref, wq_ref, wk_ref, wv_ref, q_ref, k_ref, v_ref,
    part, sums, got, got_sums, s_send, s_recv, p_send, p_recv,
):
    me = lax.axis_index("ep")
    x = x_ref[...].astype(F32)
    xg = (x * g_ref[...]).astype(BF16)
    rows = k_ref.shape[0]
    sums[...] = row_sums(x * x)
    at = 0
    for w_ref in (wq_ref, wk_ref, wv_ref):
        cols = w_ref.shape[1]
        val = jnp.dot(xg, w_ref[...], preferred_element_type=F32).astype(BF16)
        for i in range(n):
            part[i, :, at : at + cols] = val[i * rows : (i + 1) * rows]
        at += cols
    greet((("ep", n),))
    copies = []
    for k in range(1, n):
        peer = lax.rem(me + k, n)
        copies.append(send("ep", n, k, part.at[peer], got.at[k - 1], p_send, p_recv))
        copies.append(send("ep", n, k, sums, got_sums.at[k - 1], s_send, s_recv))
    total = part[me].astype(F32)
    squares = sums[...]
    for k in range(1, n):
        copies[2 * k - 2].wait_recv()
        total = total + got[k - 1].astype(F32)
        copies[2 * k - 1].wait_recv()
        squares = squares + got_sums[k - 1]
    mean = own_column(squares, me * rows, rows) / width
    total = total * lax.rsqrt(mean + EPSILON)
    hd = q_ref.shape[2]
    q_width = wq_ref.shape[1]
    k_width = wk_ref.shape[1]
    for h in range(q_ref.shape[0]):
        q_ref[h] = total[:, h * hd : (h + 1) * hd].astype(BF16).astype(F32)
    k_ref[...] = total[:, q_width : q_width + k_width].astype(BF16)
    v_ref[...] = total[:, q_width + k_width :].astype(BF16)
    for copy in copies:
        copy.wait_send()


def attend_kernel(kv, per, len_ref, off_ref, q_ref, gain_ref, new_k_ref, new_v_ref, key_ref, val_ref,
                  out_ref, k_out_ref, v_out_ref):
    step = pl.program_id(0)
    k_out_ref[...] = new_k_ref[...]
    v_out_ref[...] = new_v_ref[...]
    heads = q_ref.shape[0]
    hd = q_ref.shape[2]
    cols = key_ref.shape[1]
    group = heads // kv
    rows = per * heads
    lanes = 128
    blocks = cols // lanes
    q = jnp.concatenate(
        [q_ref[h, pl.ds(step * per + s, 1), :] for s in range(per) for h in range(heads)], axis=0
    ).astype(BF16)
    row = lax.broadcasted_iota(jnp.int32, (rows, lanes), 0)
    lane = lax.broadcasted_iota(jnp.int32, (rows, lanes), 1)
    offset = jnp.zeros((rows, lanes), F32)
    length = jnp.zeros((rows, lanes), jnp.int32)
    for s in range(per):
        length = jnp.where(row // heads == s, len_ref[step * per + s], length)
    for h in range(heads):
        offset = jnp.where(row % heads == h, off_ref[h], offset)
    mine = (row % heads) // group
    scores = jnp.zeros((rows, cols), F32)
    row_all = lax.broadcasted_iota(jnp.int32, (rows, cols), 0)
    for s in range(per):
        one = lax.dot_general(q, key_ref[s], NT, preferred_element_type=F32)
        scores = one if s == 0 else jnp.where(row_all // heads == s, one, scores)
    sigs, valids, fails = [], [], []
    for b in range(blocks):
        sc = scores[:, b * lanes : (b + 1) * lanes] * hd ** (-0.5) + offset
        col = lane + b * lanes
        valid = (col // kv < length) & (col % kv == mine)
        ls = jnp.minimum(sc, 0.0) - jnp.log(1.0 + jnp.exp(-jnp.abs(sc)))
        sigs.append(ls)
        valids.append(valid)
        fails.append(jnp.where(valid, ls - sc, 0.0))
    failed = jnp.concatenate(fails, axis=0)
    high = failed.astype(BF16)
    low = (failed - high.astype(F32)).astype(BF16)
    r = lax.broadcasted_iota(jnp.int32, (lanes, 2 * lanes), 0)
    c = lax.broadcasted_iota(jnp.int32, (lanes, 2 * lanes), 1)
    tri = jnp.where((r > c) | (c >= lanes), 1.0, 0.0).astype(BF16)
    sums = jnp.dot(high, tri, preferred_element_type=F32) + jnp.dot(
        low, tri, preferred_element_type=F32
    )
    acc = jnp.zeros((rows, lanes), F32)
    weights = [None] * blocks
    for b in reversed(range(blocks)):
        later = sums[b * rows : (b + 1) * rows, :lanes] + acc
        acc = acc + sums[b * rows : (b + 1) * rows, lanes:]
        weights[b] = jnp.where(valids[b], jnp.exp(sigs[b] + later), 0.0)
    weights = jnp.concatenate(weights, axis=1).astype(BF16)
    row_out = lax.broadcasted_iota(jnp.int32, (rows, hd), 0)
    att = None
    for s in range(per):
        one = jnp.dot(weights, val_ref[s], preferred_element_type=F32)
        att = one if s == 0 else jnp.where(row_out // heads == s, one, att)
    gains = jnp.concatenate([gain_ref[...]] * per, axis=0)
    att = att * lax.rsqrt(jnp.mean(att * att, axis=1, keepdims=True) + EPSILON) * gains
    for s in range(per):
        for h in range(heads):
            out_ref[h, pl.ds(step * per + s, 1), :] = att[s * heads + h : s * heads + h + 1]


def rest_kernel(
    n, nt, width, cap,
    head_ref, x_ref, fg_ref, mix_ref, route_ref, route_w_ref,
    wo_hbm, dg_hbm, du_hbm, dd_hbm, eg_hbm, eu_hbm, ed_hbm,
    out_ref,
    wo, dg, du, dd, eg, eu, ed, w_sem,
    heads_all, part, disp, disp_in, sums, sums_in, gu, gu_in, hid_all, act_s, share_s,
    ret_x, ret_p, ret_m, ret, ret_in, res,
    a_in, a_pair, a_cross, a_full, f_in, f_pair, f_cross, f_full,
    h_send, h_recv, d_send, d_recv, w_send, w_recv, s_send, s_recv, g_send, g_recv,
    i_send, i_recv, r_send, r_recv, a_send, a_recv, f_send, f_recv, x_send, x_recv,
):
    me = lax.axis_index("ep")
    loads = []
    for i, (src, dst) in enumerate(
        ((wo_hbm, wo), (dg_hbm, dg), (du_hbm, du), (eg_hbm.at[0], eg), (eu_hbm.at[0], eu),
         (ed_hbm.at[0], ed), (dd_hbm, dd))
    ):
        load = pltpu.make_async_copy(src, dst, w_sem.at[i])
        load.start()
        loads.append(load)
    total_rows, block = x_ref.shape
    rows = total_rows // n
    heads_all[me] = jnp.concatenate(
        [head_ref[h] for h in range(head_ref.shape[0])], axis=1
    ).astype(BF16)
    greet((("ep", n), ("tp", nt)))
    sent = []
    copies = [
        send("ep", n, k, heads_all.at[me], heads_all.at[me], h_send, h_recv) for k in range(1, n)
    ]
    sent += copies
    me_t = lax.axis_index("tp")
    core = lax.rem(me_t, 2)
    partner = me_t + 1 - 2 * core
    half = cap // 2
    near = pl.ds(pl.multiple_of(core * half, half), half)
    far = pl.ds(pl.multiple_of((1 - core) * half, half), half)
    top = route_ref.shape[0]
    expert_ids = lax.broadcasted_iota(jnp.int32, (n, total_rows), 0)
    named = [
        jnp.where(route_ref[k : k + 1, :] == expert_ids, 1.0, 0.0).astype(F32)
        for k in range(top)
    ]
    token_r = lax.broadcasted_iota(jnp.int32, (total_rows, total_rows), 0)
    token_c = lax.broadcasted_iota(jnp.int32, (total_rows, total_rows), 1)
    before = jnp.dot(
        sum(named).astype(BF16),
        jnp.where(token_r < token_c, 1.0, 0.0).astype(BF16),
        preferred_element_type=F32,
    )
    slots = [
        jnp.sum(named[k] * before, axis=0, keepdims=True)
        + route_ref[k : k + 1, :].astype(F32) * cap
        for k in range(top)
    ]
    columns = [
        jnp.sum(jnp.where(token_r == token_c, slot, 0.0), axis=1, keepdims=True)
        for slot in slots
    ]
    share_sum = route_w_ref[0:1, :]
    for k in range(1, top):
        share_sum = share_sum + route_w_ref[k : k + 1, :]
    share_rows = [route_w_ref[k : k + 1, :] / share_sum for k in range(top)]
    slot_rows = lax.broadcasted_iota(jnp.int32, (cap, total_rows), 0)
    half_rows = lax.broadcasted_iota(jnp.int32, (half, total_rows), 0) + core * half
    loads[0].wait()
    for copy in copies:
        copy.wait_recv()
    all_heads = heads_all[...].reshape(total_rows, heads_all.shape[2])
    part[...] = jnp.dot(all_heads, wo[...], preferred_element_type=F32).astype(BF16)
    tp_sum(nt, part, a_in, a_pair, a_cross, a_full, (a_send, a_recv), None)
    residual = x_ref[...].astype(F32) + a_full[...].astype(F32)
    u = (residual * fg_ref[...]).astype(BF16)
    sums[...] = row_sums(residual * residual)
    res[...] = residual

    def picks(expert, places):
        place = (places + expert * cap).astype(F32)
        return [slot == place for slot in slots]

    d_copies, s_copies = [], []
    for k in range(1, n):
        peer = lax.rem(me + k, n)
        hit = functools.reduce(jnp.logical_or, picks(peer, half_rows))
        disp[k] = jnp.dot(
            jnp.where(hit, 1.0, 0.0).astype(BF16), u, preferred_element_type=F32
        ).astype(BF16)
        d_copies.append(send("ep", n, k, disp.at[k], disp_in.at[k - 1, near], d_send, d_recv))
        s_copies.append(send("ep", n, k, sums, sums_in.at[k - 1], s_send, s_recv))
    sent += d_copies + s_copies
    mine = picks(me, slot_rows)
    hit = functools.reduce(jnp.logical_or, mine)
    own_in = jnp.dot(
        jnp.where(hit, 1.0, 0.0).astype(BF16), u, preferred_element_type=F32
    ).astype(BF16)
    hidden = dg.shape[1]
    loads[1].wait()
    val = jnp.dot(u, dg[...], preferred_element_type=F32).astype(BF16)
    for i in range(n):
        gu[i, :, :hidden] = val[i * rows : (i + 1) * rows]
    loads[2].wait()
    val = jnp.dot(u, du[...], preferred_element_type=F32).astype(BF16)
    for i in range(n):
        gu[i, :, hidden:] = val[i * rows : (i + 1) * rows]
    g_copies = [
        send("ep", n, k, gu.at[lax.rem(me + k, n)], gu_in.at[k - 1], g_send, g_recv)
        for k in range(1, n)
    ]
    sent += g_copies
    loads[3].wait()
    loads[4].wait()
    first = pl.ds(pl.multiple_of(me * block, block), block)
    gate = jnp.dot(own_in, eg[first, :], preferred_element_type=F32)
    up = jnp.dot(own_in, eu[first, :], preferred_element_type=F32)
    squares = sums[...]
    forwards = []
    for k in range(1, n + 1):
        if k < n:
            d_copies[k - 1].wait_recv()
            forwards.append(
                send_to(
                    partner, disp_in.at[k - 1, near], disp_in.at[k - 1, near],
                    (w_send, w_recv), k - 1,
                )
            )
        if k > 1:
            p = k - 1
            s_copies[p - 1].wait_recv()
            squares = squares + sums_in[p - 1]
            forwards[p - 1].wait_recv()
            owner = lax.rem(me - p + n, n)
            span = pl.ds(pl.multiple_of(owner * block, block), block)
            gate = gate + jnp.dot(disp_in[p - 1], eg[span, :], preferred_element_type=F32)
            up = up + jnp.dot(disp_in[p - 1], eu[span, :], preferred_element_type=F32)
    sent += forwards
    scale_row = lax.rsqrt(squares[0:1, :] / width + EPSILON)
    scale = jnp.sum(jnp.where(hit, scale_row, 0.0), axis=1, keepdims=True)
    share = jnp.zeros((cap, 1), F32)
    for k in range(len(mine)):
        share = share + jnp.sum(
            jnp.where(mine[k], share_rows[k], 0.0), axis=1, keepdims=True
        )
    gate = gate * scale
    up = up * scale
    act_s[...] = (gate / (1.0 + jnp.exp(-gate)) * up).astype(BF16)
    share_s[...] = jnp.broadcast_to(share, share_s.shape)
    loads[5].wait()
    act_far = act_s[far]
    share_far = share_s[far][:, 0:1]
    for i in range(n):
        ret_x[i] = (
            jnp.dot(act_far, ed[:, i * block : (i + 1) * block], preferred_element_type=F32)
            * share_far
        ).astype(BF16)
    swap = send_to(partner, ret_x, ret_p, (x_send, x_recv), 0)
    sent.append(swap)
    act_near = act_s[near]
    share_near = share_s[near][:, 0:1]
    for i in range(n):
        ret_m[i] = (
            jnp.dot(act_near, ed[:, i * block : (i + 1) * block], preferred_element_type=F32)
            * share_near
        )
    swap.wait_recv()
    for i in range(n):
        ret[i] = (ret_m[i] + ret_p[i].astype(F32)).astype(BF16)
    r_copies = [
        send("ep", n, k, ret.at[lax.rem(me + k, n)], ret_in.at[k - 1], r_send, r_recv)
        for k in range(1, n)
    ]
    sent += r_copies
    gate_up = gu[me].astype(F32)
    for k in range(1, n):
        g_copies[k - 1].wait_recv()
        gate_up = gate_up + gu_in[k - 1].astype(F32)
    gate_up = gate_up * own_column(
        jnp.broadcast_to(scale_row, (8, total_rows)), me * rows, rows
    )
    dense_gate = gate_up[:, :hidden]
    hid_all[me] = (dense_gate / (1.0 + jnp.exp(-dense_gate)) * gate_up[:, hidden:]).astype(BF16)
    i_copies = [
        send("ep", n, k, hid_all.at[me], hid_all.at[me], i_send, i_recv) for k in range(1, n)
    ]
    sent += i_copies
    slot_cols = lax.broadcasted_iota(jnp.int32, (total_rows, half), 1) + core * half
    def combine(expert, rows_in):
        place = (slot_cols + expert * cap).astype(F32)
        hits = functools.reduce(jnp.logical_or, [column == place for column in columns])
        return jnp.dot(
            jnp.where(hits, 1.0, 0.0).astype(BF16), rows_in, preferred_element_type=F32
        )

    moe = combine(me, ret[me])
    for k in range(1, n):
        r_copies[k - 1].wait_recv()
        moe = moe + combine(lax.rem(me - k + n, n), ret_in[k - 1])
    loads[6].wait()
    for copy in i_copies:
        copy.wait_recv()
    dense = jnp.dot(
        hid_all[...].reshape(total_rows, hidden), dd[...], preferred_element_type=F32
    )
    both = moe + mix_ref[...] * dense
    part[...] = both.astype(BF16)
    tp_sum(nt, part, f_in, f_pair, f_cross, f_full, (f_send, f_recv), res)
    out_ref[...] = f_full[...]
    for copy in sent:
        copy.wait_send()


def per_device(
    n, nt, stream, norm_gain, w_query, w_key, w_value, break_offset, cache_keys, cache_values,
    lengths, w_output, head_gain, ffn_gain, route_experts, route_weights, expert_gate,
    expert_up, expert_down, dense_gate, dense_up, dense_down, mix_gain,
):
    total_rows, block = stream.shape
    width = block * n
    rows = lengths.shape[0]
    kv = cache_keys.shape[2]
    hd = cache_keys.shape[3]
    heads = break_offset.shape[0]
    cache_len = cache_keys.shape[1]
    top = route_experts.shape[1]
    hidden = dense_gate.shape[1]
    expert_hidden = expert_gate.shape[2]
    experts = expert_gate.shape[0] * n
    cap = 2 * rows * top // expert_gate.shape[0]
    assert experts == n
    vmem = pl.BlockSpec(memory_space=pltpu.VMEM)
    hbm = pl.BlockSpec(memory_space=pl.ANY)
    dma = pltpu.SemaphoreType.DMA
    limit = 60 * 1024 * 1024

    wide = w_query.shape[1] + w_key.shape[1] + w_value.shape[1]
    queries, key_rows, value_rows = pl.pallas_call(
        functools.partial(project_kernel, n, width),
        out_shape=(
            jax.ShapeDtypeStruct((heads, rows, hd), F32),
            jax.ShapeDtypeStruct((rows, w_key.shape[1]), BF16),
            jax.ShapeDtypeStruct((rows, w_value.shape[1]), BF16),
        ),
        in_specs=[vmem] * 5,
        out_specs=(vmem, vmem, vmem),
        scratch_shapes=[
            pltpu.VMEM((n, rows, wide), BF16),
            pltpu.VMEM((8, total_rows), F32),
            pltpu.VMEM((n - 1, rows, wide), BF16),
            pltpu.VMEM((n - 1, 8, total_rows), F32),
            dma((n - 1,)), dma((n - 1,)), dma((n - 1,)), dma((n - 1,)),
        ],
        compiler_params=pltpu.CompilerParams(collective_id=0, has_side_effects=True),
        name="project",
    )(stream, norm_gain.reshape(1, block), w_query, w_key, w_value)

    per = 2
    flat = kv * cache_len
    smem = pl.BlockSpec(memory_space=pltpu.SMEM)
    k_block = pl.BlockSpec(key_rows.shape, lambda i: (0, 0))
    v_block = pl.BlockSpec(value_rows.shape, lambda i: (0, 0))
    head_out, key_rows, value_rows = pl.pallas_call(
        functools.partial(attend_kernel, kv, per),
        grid=(rows // per,),
        out_shape=(
            jax.ShapeDtypeStruct((heads, rows, hd), F32),
            jax.ShapeDtypeStruct(key_rows.shape, BF16),
            jax.ShapeDtypeStruct(value_rows.shape, BF16),
        ),
        in_specs=[
            smem,
            smem,
            pl.BlockSpec((heads, rows, hd), lambda i: (0, 0, 0)),
            pl.BlockSpec((heads, hd), lambda i: (0, 0)),
            k_block,
            v_block,
            pl.BlockSpec((per, flat, hd), lambda i: (i, 0, 0)),
            pl.BlockSpec((per, flat, hd), lambda i: (i, 0, 0)),
        ],
        out_specs=(pl.BlockSpec((heads, rows, hd), lambda i: (0, 0, 0)), k_block, v_block),
        compiler_params=pltpu.CompilerParams(dimension_semantics=("arbitrary",)),
        name="attend",
    )(
        lengths,
        break_offset,
        queries,
        head_gain.reshape(heads, hd),
        key_rows,
        value_rows,
        cache_keys.reshape(rows, flat, hd),
        cache_values.reshape(rows, flat, hd),
    )

    dt = w_output.shape[0]
    assert nt % 2 == 0 and cap % 2 == 0
    half_cap = (n, cap // 2, block)
    half_rows = (total_rows // 2, block)
    mixed_out = pl.pallas_call(
        functools.partial(rest_kernel, n, nt, width, cap),
        out_shape=jax.ShapeDtypeStruct((total_rows, block), BF16),
        in_specs=[vmem] * 6 + [hbm] * 7,
        out_specs=vmem,
        scratch_shapes=[
            pltpu.VMEM(w_output.shape, BF16),
            pltpu.VMEM(dense_gate.shape, BF16),
            pltpu.VMEM(dense_up.shape, BF16),
            pltpu.VMEM(dense_down.shape, BF16),
            pltpu.VMEM(expert_gate.shape[1:], BF16),
            pltpu.VMEM(expert_up.shape[1:], BF16),
            pltpu.VMEM(expert_down.shape[1:], BF16),
            dma((7,)),
            pltpu.VMEM((n, rows, dt), BF16),
            pltpu.VMEM((total_rows, block), BF16),
            pltpu.VMEM(half_cap, BF16),
            pltpu.VMEM((n - 1, cap, block), BF16),
            pltpu.VMEM((8, total_rows), F32),
            pltpu.VMEM((n - 1, 8, total_rows), F32),
            pltpu.VMEM((n, rows, 2 * hidden), BF16),
            pltpu.VMEM((n - 1, rows, 2 * hidden), BF16),
            pltpu.VMEM((n, rows, hidden), BF16),
            pltpu.VMEM((cap, expert_hidden), BF16),
            pltpu.VMEM((cap, 128), F32),
            pltpu.VMEM(half_cap, BF16),
            pltpu.VMEM(half_cap, BF16),
            pltpu.VMEM(half_cap, F32),
            pltpu.VMEM(half_cap, BF16),
            pltpu.VMEM((n - 1, cap // 2, block), BF16),
            pltpu.VMEM((total_rows, block), F32),
        ]
        + [
            pltpu.VMEM(half_rows, BF16),
            pltpu.VMEM(half_rows, BF16),
            pltpu.VMEM((nt // 2 - 1,) + half_rows, BF16),
            pltpu.VMEM((total_rows, block), BF16),
        ] * 2
        + [dma((n - 1,))] * 14
        + [dma((nt // 2 + 1,))] * 4
        + [
            dma((1,)),
            dma((1,)),
        ],
        compiler_params=pltpu.CompilerParams(
            collective_id=1, has_side_effects=True, vmem_limit_bytes=limit
        ),
        name="rest",
    )(
        head_out, stream, ffn_gain.reshape(1, block), mix_gain.reshape(1, block),
        route_experts.T, route_weights.T,
        w_output, dense_gate, dense_up, dense_down, expert_gate, expert_up, expert_down,
    )
    return (mixed_out, key_rows, value_rows)


def solution(mesh):
    in_specs = (
        P(None, "ep"),
        P("ep"),
        P("ep", "tp"),
        P("ep", "tp"),
        P("ep", "tp"),
        P("tp"),
        P("ep", None, "tp", None),
        P("ep", None, "tp", None),
        P("ep"),
        P("tp", "ep"),
        P("tp"),
        P("ep"),
        P(),
        P(),
        P("ep", None, "tp"),
        P("ep", None, "tp"),
        P("ep", "tp", None),
        P("ep", "tp"),
        P("ep", "tp"),
        P("tp", "ep"),
        P("ep"),
    )
    out_specs = (P(None, "ep"), P("ep", "tp"), P("ep", "tp"))
    body = functools.partial(per_device, mesh.shape["ep"], mesh.shape["tp"])
    return jax.shard_map(
        body, mesh=mesh, in_specs=in_specs, out_specs=out_specs, check_vma=False
    )
```
